32 devices in a mesh: sp: 8 (over z, x), tp: 4 (over y, core).
Axes of the slice: x: 2, y: 2, z: 4, core: 2. Of those that a mesh axis runs over, the one named last changes fastest.
Arguments:
- query_narrow: bfloat16 [2048, 1024], P('sp', 'tp'), may hold values from -6 to 6
- key_narrow: bfloat16 [2048, 1024], P('sp', 'tp'), may hold values from -6 to 6
- value_narrow: bfloat16 [2048, 1024], P('sp', 'tp'), may hold values from -12 to 12
- query_broad: bfloat16 [2048, 1024], P('sp', 'tp'), may hold values from -6 to 6
- key_broad: bfloat16 [2048, 1024], P('sp', 'tp'), may hold values from -6 to 6
- value_broad: bfloat16 [2048, 1024], P('sp', 'tp'), may hold values from -12 to 12
- offset_narrow: bfloat16 [16, 2048], P('tp', 'sp'), as said below
- offset_broad: bfloat16 [8, 2048], P('tp', 'sp'), as said below
- residual: bfloat16 [2048, 2048], P(('sp', 'tp')), may hold values from -6 to 6
- out_narrow: bfloat16 [1024, 2048], P('tp'), may hold values from -0.25 to 0.25
- out_broad: bfloat16 [1024, 2048], P('tp'), may hold values from -0.25 to 0.25
- norm_gain: float32 [2048], replicated, may hold values from 0.1 to 1.9
- up_proj: bfloat16 [2048, 8192], P('sp', 'tp'), may hold values from -0.125 to 0.125
- down_proj: bfloat16 [8192, 2048], P('tp', 'sp'), may hold values from -0.0625 to 0.0625
Outputs:
- output: bfloat16 [2048, 2048], P(('sp', 'tp'))
The draws below stay inside these ranges and needn't reach their ends.
Inputs may be any that keep to these rules, and one draw needn't show every extreme that they name: `offset_narrow`: additive score offsets of each head for each key position. `offset_broad`: additive score offsets of each head for each key position.
All inputs are finite; a program needn't handle non-finite values.
Results may differ from the reference program's by a relative error of at most 0.018.
Values may be sent and summed in bfloat16 or wider, within the bound.
A program may use at most 64 MiB of HBM per device.

```python
import math
import jax
import jax.numpy as jnp
from jax import lax

D = 2048
FF = 8192
NARROW_HEADS = 16
NARROW_SIZE = 64
BROAD_HEADS = 8
BROAD_SIZE = 128
TOKENS_PER_SHARD = 256
SEQUENCE_TOKENS = 2048


def stick_offsets(key, total_heads, salt):
    key = jax.random.fold_in(key, salt)
    random_subkeys = jax.random.split(key, 6)
    gradual_drift = jax.random.randint(random_subkeys[0], (total_heads, 1), 0, 2).astype(jnp.float32)
    slow_base = -jnp.log(jnp.float32(SEQUENCE_TOKENS)) - 2.0
    fast_base = -jnp.log(jnp.float32(40.0)) - 0.5
    base_value = gradual_drift * slow_base + (1.0 - gradual_drift) * fast_base
    base_value = base_value + jax.random.uniform(random_subkeys[1], (total_heads, 1), jnp.float32, -0.3, 0.3)
    slope_factor = jax.random.uniform(random_subkeys[2], (total_heads, SEQUENCE_TOKENS // TOKENS_PER_SHARD), jnp.float32, -0.7, 0.7)
    slope_factor = jnp.repeat(slope_factor, TOKENS_PER_SHARD, axis=1)
    jagged_noise = 0.5 * jax.random.truncated_normal(random_subkeys[3], -2.0, 2.0, (total_heads, SEQUENCE_TOKENS), jnp.float32)
    spike_amount = (jax.random.randint(random_subkeys[4], (total_heads, SEQUENCE_TOKENS), 0, 2 * TOKENS_PER_SHARD) == 0).astype(jnp.float32) * gradual_drift
    spike_height = jax.random.uniform(random_subkeys[5], (total_heads, SEQUENCE_TOKENS), jnp.float32, -1.9, -0.9)
    shift_amount = spike_amount * spike_height + (1.0 - spike_amount) * (base_value + slope_factor + jagged_noise)
    return shift_amount.astype(jnp.bfloat16)


def draw_offset_narrow(key, part):
    return stick_offsets(key, NARROW_HEADS, 11)


def draw_offset_broad(key, part):
    return stick_offsets(key, BROAD_HEADS, 23)


def level_of(own_key, shape, cuts, low, top_value):
    factor_of, own = 1.0, jax.random.fold_in(own_key, 6)
    for dim, parts in cuts:
        draws = jnp.exp(jax.random.uniform(jax.random.fold_in(own, dim), (parts,), jnp.float32, low / len(cuts), top_value / len(cuts)))
        factor_of = factor_of * jnp.repeat(draws, shape[dim] // parts).reshape([-1 if axis == dim else 1 for axis in range(len(shape))])
    return factor_of


def centred(stream_key, extent, spread, bound, pieces=(), held_as=jnp.bfloat16):
    result = spread * jax.random.normal(stream_key, extent, jnp.float32)
    if pieces:
        result = result * level_of(stream_key, extent, pieces, -0.22, 0.18)
    return jnp.clip(result, -bound, bound).astype(held_as)


def setup_inputs(seed: int = 0) -> dict:
    arg_keys = jax.random.split(jax.random.key(seed), 15)
    query_narrow = centred(arg_keys[0], (SEQUENCE_TOKENS, NARROW_HEADS * NARROW_SIZE), 1.0, 6.0, ((0, 8), (1, 4)))
    key_narrow = centred(arg_keys[1], (SEQUENCE_TOKENS, NARROW_HEADS * NARROW_SIZE), 1.0, 6.0, ((0, 8), (1, 4)))
    value_narrow = centred(arg_keys[2], (SEQUENCE_TOKENS, NARROW_HEADS * NARROW_SIZE), 2.0, 12.0, ((0, 8), (1, 4)))
    query_broad = centred(arg_keys[3], (SEQUENCE_TOKENS, BROAD_HEADS * BROAD_SIZE), 1.0, 6.0, ((0, 8), (1, 4)))
    key_broad = centred(arg_keys[4], (SEQUENCE_TOKENS, BROAD_HEADS * BROAD_SIZE), 1.0, 6.0, ((0, 8), (1, 4)))
    value_broad = centred(arg_keys[5], (SEQUENCE_TOKENS, BROAD_HEADS * BROAD_SIZE), 2.0, 12.0, ((0, 8), (1, 4)))
    offset_narrow = draw_offset_narrow(jax.random.fold_in(arg_keys[14], 71), 0)
    offset_broad = draw_offset_broad(jax.random.fold_in(arg_keys[14], 71), 0)
    residual = centred(arg_keys[8], (SEQUENCE_TOKENS, D), 1.0, 6.0, ((0, 32),))
    out_narrow = centred(arg_keys[9], (NARROW_HEADS * NARROW_SIZE, D), ((NARROW_HEADS * NARROW_SIZE + BROAD_HEADS * BROAD_SIZE) // 4) ** -0.5, 0.25, ((0, 4),))
    out_broad = centred(arg_keys[10], (BROAD_HEADS * BROAD_SIZE, D), ((NARROW_HEADS * NARROW_SIZE + BROAD_HEADS * BROAD_SIZE) // 4) ** -0.5, 0.25, ((0, 4),))
    norm_gain = jnp.clip(1.0 + 0.18 * jax.random.normal(arg_keys[11], (D,), jnp.float32), 0.1, 1.9)
    up_proj = centred(arg_keys[12], (D, FF), D ** -0.5, 0.125, ((0, 8), (1, 4)))
    down_proj = centred(arg_keys[13], (FF, D), FF ** -0.5, 0.0625, ((0, 4), (1, 8)))
    return {"query_narrow": query_narrow, "key_narrow": key_narrow, "value_narrow": value_narrow, "query_broad": query_broad, "key_broad": key_broad, "value_broad": value_broad, "offset_narrow": offset_narrow, "offset_broad": offset_broad, "residual": residual, "out_narrow": out_narrow, "out_broad": out_broad, "norm_gain": norm_gain, "up_proj": up_proj, "down_proj": down_proj}


def stick_group(query, key, value, shift_amount, total_heads, head_size):
    tokens = query.shape[0]
    span_rows = math.gcd(tokens, 512)
    blocks = tokens // span_rows
    q_all = query.astype(jnp.float32).reshape(tokens, total_heads, head_size)
    k_all = key.astype(jnp.float32).reshape(tokens, total_heads, head_size)
    v_all = value.astype(jnp.float32).reshape(tokens, total_heads, head_size)
    off_all = shift_amount.astype(jnp.float32)

    def query_block(index):
        q_start = index * span_rows
        q_block = lax.dynamic_slice_in_dim(q_all, q_start, span_rows, 0)
        query_pos = q_start + jnp.arange(span_rows, dtype=jnp.int32)

        def key_block(turn_index, state):
            keep_sum, running = state
            k_start = (index - turn_index) * span_rows
            k_block = lax.dynamic_slice_in_dim(k_all, k_start, span_rows, 0)
            v_block = lax.dynamic_slice_in_dim(v_all, k_start, span_rows, 0)
            o_block = lax.dynamic_slice_in_dim(off_all, k_start, span_rows, 1)
            key_pos = k_start + jnp.arange(span_rows, dtype=jnp.int32)
            scores = jnp.einsum('qhe,khe->hqk', q_block, k_block) * head_size ** (-0.5) + o_block[:, None, :]
            causal = (key_pos[None, :] < query_pos[:, None])[None]
            log_keep = jnp.where(causal, jax.nn.log_sigmoid(-scores), jnp.float32(0.0))
            keep_after = lax.cumsum(log_keep, axis=2, reverse=True) - log_keep
            weight = jnp.where(causal, jnp.exp(jax.nn.log_sigmoid(scores) + keep_after + keep_sum[:, :, None]), jnp.float32(0.0))
            rounded = lax.optimization_barrier(weight.astype(jnp.bfloat16)).astype(jnp.float32)
            running = running + jnp.einsum('hqk,khe->qhe', rounded, v_block)
            return (keep_sum + lax.optimization_barrier(jnp.sum(log_keep, axis=2)), running)
        start_state = (jnp.zeros((total_heads, span_rows), jnp.float32), jnp.zeros((span_rows, total_heads, head_size), jnp.float32))
        keep_sum, running = lax.fori_loop(jnp.int32(0), index + 1, key_block, start_state)
        return running.reshape(span_rows, total_heads * head_size)
    mixed = lax.map(query_block, jnp.arange(blocks, dtype=jnp.int32))
    return mixed.reshape(tokens, total_heads * head_size).astype(jnp.bfloat16)

def reference(query_narrow, key_narrow, value_narrow, query_broad, key_broad, value_broad, offset_narrow, offset_broad, residual, out_narrow, out_broad, norm_gain, up_proj, down_proj):
    mixed_narrow = stick_group(query_narrow, key_narrow, value_narrow, offset_narrow, NARROW_HEADS, NARROW_SIZE)
    mixed_broad = stick_group(query_broad, key_broad, value_broad, offset_broad, BROAD_HEADS, BROAD_SIZE)
    attended = jnp.dot(mixed_narrow, out_narrow, preferred_element_type=jnp.float32) + jnp.dot(mixed_broad, out_broad, preferred_element_type=jnp.float32)
    updated = residual.astype(jnp.float32) + attended
    scale = lax.rsqrt(lax.optimization_barrier(jnp.mean(updated * updated, axis=-1, keepdims=True)) + 1e-06)
    normed = (updated * scale * norm_gain).astype(jnp.bfloat16)
    hidden = jnp.square(jax.nn.relu(jnp.dot(normed, up_proj, preferred_element_type=jnp.float32))).astype(jnp.bfloat16)
    return (updated + jnp.dot(hidden, down_proj, preferred_element_type=jnp.float32)).astype(jnp.bfloat16)
```

```python
import functools

import jax
import jax.numpy as jnp
from jax import lax
from jax.experimental import pallas as pl
from jax.experimental.pallas import tpu as pltpu
from jax.sharding import PartitionSpec as P

NARROW_SIZE = 64
BROAD_SIZE = 128
F32 = jnp.float32
BF16 = jnp.bfloat16


def ring_order(shards):
    across = 1 << ((shards.bit_length() - 1) // 2)
    along = shards // across
    order = [z * across for z in range(along)]
    for turn, z in enumerate(reversed(range(along))):
        row = list(range(1, across))
        if turn % 2:
            row.reverse()
        order += [z * across + x for x in row]
    return order


def lookup(table, index):
    found = jnp.int32(0)
    for place, value in enumerate(table):
        found = found + jnp.where(index == place, jnp.int32(value), jnp.int32(0))
    return found


def kernel(
    shards, peers, order,
    q_n, q_b, k_n, v_n, k_b, v_b, off_n, off_b, residual, out_n, out_b, gain, up, down,
    o_ref,
    kv_slots, off_slots, up_slots, down_slots, mixed, part, inbox, updated, normed_all,
    product, hidden, channel, send_sems, recv_sems, tp_send, tp_recv, load_sems,
):
    tok = q_n.shape[0]
    wide = product.shape[1]
    model = part.shape[2]
    rows = residual.shape[0]
    depth = up.shape[0]
    me = lax.axis_index("sp")
    me_tp = lax.axis_index("tp")
    inverse = [order.index(s) for s in range(shards)]
    pos = lookup(inverse, me)
    right = lookup(order, lax.rem(pos + 1, shards))
    left = lookup(order, lax.rem(pos + shards - 1, shards))

    half_up, half_down = wide // 2, wide // 2
    loads = []
    for way, (k, v, off) in enumerate(((k_n, v_n, off_n), (k_b, v_b, off_b))):
        loads += [
            (k, kv_slots.at[way, 0, pl.ds(0, tok)]),
            (v, kv_slots.at[way, 0, pl.ds(tok, tok)]),
            (off, off_slots.at[way, 0]),
        ]
    for way in range(2):
        loads += [
            (up.at[:, pl.ds(way * half_up, half_up)], up_slots.at[way, 0]),
            (down.at[pl.ds(way * half_down, half_down)], down_slots.at[way, 0]),
        ]
    loads = [
        pltpu.make_async_copy(src, dst, load_sems.at[i]) for i, (src, dst) in enumerate(loads)
    ]
    for load in loads:
        load.start()

    barrier = pltpu.get_barrier_semaphore()
    for shard in (left, right):
        pl.semaphore_signal(
            barrier, inc=1, device_id=(shard, me_tp), device_id_type=pl.DeviceIdType.MESH
        )
    for d in range(1, peers):
        pl.semaphore_signal(
            barrier, inc=1, device_id=(me, lax.rem(me_tp + d, peers)),
            device_id_type=pl.DeviceIdType.MESH,
        )
    pl.semaphore_wait(barrier, 1 + peers)

    def piece(stream, way, t):
        if stream == 0:
            return kv_slots.at[way, t]
        if stream == 1:
            return off_slots.at[way, t]
        if stream in (2, 3):
            size = depth // 2
            return up_slots.at[way, t, pl.ds((stream - 2) * size, size)]
        size = half_down // 2
        return down_slots.at[way, t, pl.ds((stream - 4) * size, size)]

    def hop(stream, way, t):
        return pltpu.make_async_remote_copy(
            src_ref=piece(stream, way, t),
            dst_ref=piece(stream, way, t + 1),
            send_sem=send_sems.at[way, stream, t],
            recv_sem=recv_sems.at[way, stream, t],
            device_id=((left if way else right), me_tp),
            device_id_type=pl.DeviceIdType.MESH,
        )

    def begin(streams, t):
        for stream in streams:
            for way in range(2):
                hop(stream, way, t).start()

    def relay(streams, t):
        for stream in streams:
            for way in range(2):
                hop(stream, way, t - 1).wait_recv()
                hop(stream, way, t).start()

    def arrive(streams):
        for stream in streams:
            for way in range(2):
                hop(stream, way, shards - 2).wait_recv()

    def each(first, last, body):
        def step(t, carry):
            body(t)
            return carry

        lax.fori_loop(first, last, step, 0)

    KEYS, UPS, DOWNS = (0, 1), (2, 3), (4, 5)
    for load in loads:
        load.wait()
    begin(KEYS, 0)
    each(1, shards - 1, functools.partial(relay, KEYS))
    begin(UPS, 0)
    arrive(KEYS)

    row_at = lax.broadcasted_iota(jnp.int32, (tok, tok), 0)
    col_at = lax.broadcasted_iota(jnp.int32, (tok, tok), 1)
    later = (row_at > col_at).astype(BF16)
    later2 = jnp.concatenate([later, later], axis=0)
    heads = []
    for way, (q, size) in enumerate(((q_n, NARROW_SIZE), (q_b, BROAD_SIZE))):
        for h in range(q.shape[1] // size):
            heads.append((way, h, size, q))

    def head_block(way, h, size, q, block, keep_sum, diagonal):
        there = lookup(inverse, block)
        slot = lax.rem((there - pos if way else pos - there) + shards, shards)
        cols = pl.ds(h * size, size)
        keys = kv_slots[way, slot, pl.ds(0, tok), cols]
        values = kv_slots[way, slot, pl.ds(tok, tok), cols]
        offset = off_slots[way, slot].astype(F32)[h : h + 1, :]
        scores = lax.dot_general(
            q[:, cols], keys, (((1,), (1,)), ((), ())), preferred_element_type=F32
        ) * (size ** -0.5) + offset
        keep = -(jnp.maximum(scores, 0.0) + jnp.log(1.0 + jnp.exp(-jnp.abs(scores))))
        breaks = scores + keep
        if diagonal:
            keep = jnp.where(col_at < row_at, keep, 0.0)
        high = keep.astype(BF16)
        low = (keep - high.astype(F32)).astype(BF16)
        after = jnp.dot(
            jnp.concatenate([high, low], axis=1), later2, preferred_element_type=F32
        )
        weight = jnp.exp(breaks + after + keep_sum)
        if diagonal:
            weight = jnp.where(col_at < row_at, weight, 0.0)
        added = jnp.dot(weight.astype(BF16), values, preferred_element_type=F32)
        return keep_sum + (after[:, :1] + keep[:, :1]), added

    for index, (way, h, size, q) in enumerate(heads):
        start = head_block(way, h, size, q, me, jnp.zeros((tok, 1), F32), True)

        def sweep(turn, state, way=way, h=h, size=size, q=q):
            keep_sum, running = state
            keep_sum, added = head_block(way, h, size, q, me - 1 - turn, keep_sum, False)
            return keep_sum, running + added

        _, running = lax.fori_loop(0, me, sweep, start)
        base = way * q_n.shape[1] + h * size
        mixed[:, pl.ds(base, size)] = running.astype(BF16)

    relay(UPS, 1)

    def tp_copy(src, dst, kind, d):
        return pltpu.make_async_remote_copy(
            src_ref=src, dst_ref=dst,
            send_sem=tp_send.at[kind, d - 1], recv_sem=tp_recv.at[kind, d - 1],
            device_id=(me, lax.rem(me_tp + d, peers)),
            device_id_type=pl.DeviceIdType.MESH,
        )

    def scatter(kind):
        copies = []
        for d in range(1, peers):
            peer = lax.rem(me_tp + d, peers)
            copies.append(
                tp_copy(
                    part.at[kind, pl.ds(pl.multiple_of(peer * rows, rows), rows)],
                    inbox.at[kind, d - 1], kind, d,
                )
            )
        for copy in copies:
            copy.start()
        return copies

    def summed(kind, copies):
        for copy in copies:
            copy.wait_recv()
        own = pl.multiple_of(me_tp * rows, rows)
        total = part[kind, pl.ds(own, rows), :].astype(F32)
        for d in range(1, peers):
            total = total + inbox[kind, d - 1].astype(F32)
        return total

    tile = min(512, model)
    n_cols = out_n.shape[0]

    def project(c):
        cols = pl.ds(pl.multiple_of(c * tile, tile), tile)
        part[0, :, cols] = (
            jnp.dot(mixed[:, :n_cols], out_n[:, cols], preferred_element_type=F32)
            + jnp.dot(mixed[:, n_cols:], out_b[:, cols], preferred_element_type=F32)
        ).astype(BF16)

    each(0, model // tile, project)
    first = scatter(0)
    relay(UPS, 2)
    updated[...] = residual[...].astype(F32) + summed(0, first)
    value = updated[...]
    scale = lax.rsqrt(jnp.mean(value * value, axis=-1, keepdims=True) + 1e-06)
    mine = pl.ds(pl.multiple_of(me_tp * rows, rows), rows)
    normed_all[mine, :] = (value * scale * gain[...]).astype(BF16)
    spread = [tp_copy(normed_all.at[mine], normed_all.at[mine], 2, d) for d in range(1, peers)]
    for copy in spread:
        copy.start()
    relay(UPS, 3)
    for copy in spread:
        copy.wait_recv()

    product[...] = jnp.zeros_like(product)
    channel[...] = jnp.zeros_like(channel)
    step_cols = min(512, half_up)

    def source(way, t):
        return lookup(order, lax.rem((pos + t if way else pos - t + shards), shards))

    def climb(t):
        for way in range(2):
            lhs_cols = pl.ds(pl.multiple_of(source(way, t) * depth, depth), depth)

            def one(c, way=way, lhs_cols=lhs_cols):
                at = pl.multiple_of(c * step_cols, step_cols)
                product[:, pl.ds(way * half_up + at, step_cols)] += jnp.dot(
                    normed_all[:, lhs_cols], up_slots[way, t, :, pl.ds(at, step_cols)],
                    preferred_element_type=F32,
                )

            each(0, half_up // step_cols, one)

    def descend(t):
        for way in range(2):
            cols = pl.ds(pl.multiple_of(source(way, t) * depth, depth), depth)
            channel[:, cols] += jnp.dot(
                hidden[:, pl.ds(way * half_down, half_down)], down_slots[way, t],
                preferred_element_type=F32,
            )

    each(0, 4, climb)

    def up_step(t):
        relay(UPS, t)
        climb(t)

    each(4, shards - 1, up_step)
    begin(DOWNS, 0)
    arrive(UPS)
    climb(shards - 1)

    def activate(c):
        cols = pl.ds(pl.multiple_of(c * step_cols, step_cols), step_cols)
        hidden[:, cols] = jnp.square(jnp.maximum(product[:, cols], 0.0)).astype(BF16)

    each(0, wide // step_cols, activate)
    descend(0)

    def down_step(t):
        relay(DOWNS, t)
        descend(t)

    each(1, shards - 1, down_step)
    arrive(DOWNS)
    descend(shards - 1)

    def settle(c):
        cols = pl.ds(pl.multiple_of(c * tile, tile), tile)
        part[1, :, cols] = channel[:, cols].astype(BF16)

    each(0, model // tile, settle)
    last = scatter(1)
    o_ref[...] = (updated[...] + summed(1, last)).astype(BF16)

    def drain(t):
        for stream in KEYS + UPS + DOWNS:
            for way in range(2):
                hop(stream, way, t).wait_send()

    each(0, shards - 1, drain)
    for copy in first + spread + last:
        copy.wait_send()


def local(
    shards, peers, order,
    query_narrow, key_narrow, value_narrow, query_broad, key_broad, value_broad,
    offset_narrow, offset_broad, residual, out_narrow, out_broad, norm_gain, up_proj, down_proj,
):
    tok, columns = query_narrow.shape
    rows, model = residual.shape
    depth, wide = up_proj.shape
    pad = 16

    def padded(offset):
        return jnp.pad(offset, ((0, pad - offset.shape[0]), (0, 0)))

    vmem = pl.BlockSpec(memory_space=pltpu.VMEM)
    anywhere = pl.BlockSpec(memory_space=pl.ANY)
    return pl.pallas_call(
        functools.partial(kernel, shards, peers, order),
        out_shape=jax.ShapeDtypeStruct((rows, model), BF16),
        in_specs=[vmem] * 2 + [anywhere] * 6 + [vmem] * 4 + [anywhere] * 2,
        out_specs=vmem,
        scratch_shapes=[
            pltpu.VMEM((2, shards, 2 * tok, columns), BF16),
            pltpu.VMEM((2, shards, pad, tok), BF16),
            pltpu.VMEM((2, shards, depth, wide // 2), BF16),
            pltpu.VMEM((2, shards, wide // 2, depth), BF16),
            pltpu.VMEM((tok, 2 * columns), BF16),
            pltpu.VMEM((2, tok, model), BF16),
            pltpu.VMEM((2, peers - 1, rows, model), BF16),
            pltpu.VMEM((rows, model), F32),
            pltpu.VMEM((tok, model), BF16),
            pltpu.VMEM((tok, wide), F32),
            pltpu.VMEM((tok, wide), BF16),
            pltpu.VMEM((tok, model), F32),
            pltpu.SemaphoreType.DMA((2, 6, shards)),
            pltpu.SemaphoreType.DMA((2, 6, shards)),
            pltpu.SemaphoreType.DMA((3, peers - 1)),
            pltpu.SemaphoreType.DMA((3, peers - 1)),
            pltpu.SemaphoreType.DMA((10,)),
        ],
        compiler_params=pltpu.CompilerParams(
            collective_id=0, has_side_effects=True, vmem_limit_bytes=60 << 20
        ),
    )(
        query_narrow, query_broad, key_narrow, value_narrow, key_broad, value_broad,
        padded(offset_narrow), padded(offset_broad), residual, out_narrow, out_broad,
        norm_gain.reshape(1, -1), up_proj, down_proj,
    )


def solution(mesh):
    shards, peers = mesh.shape["sp"], mesh.shape["tp"]
    return jax.shard_map(
        functools.partial(local, shards, peers, tuple(ring_order(shards))),
        mesh=mesh,
        in_specs=(
            P("sp", "tp"),
            P("sp", "tp"),
            P("sp", "tp"),
            P("sp", "tp"),
            P("sp", "tp"),
            P("sp", "tp"),
            P("tp", "sp"),
            P("tp", "sp"),
            P(("sp", "tp"), None),
            P("tp", None),
            P("tp", None),
            P(),
            P("sp", "tp"),
            P("tp", "sp"),
        ),
        out_specs=P(("sp", "tp"), None),
        check_vma=False,
    )
```

```python
import functools

import jax
import jax.numpy as jnp
from jax import lax
from jax.experimental import pallas as pl
from jax.experimental.pallas import tpu as pltpu
from jax.sharding import PartitionSpec as P

NARROW_SIZE = 64
BROAD_SIZE = 128
F32 = jnp.float32
BF16 = jnp.bfloat16


def ring_order(shards):
    across = 1 << ((shards.bit_length() - 1) // 2)
    along = shards // across
    order = [z * across for z in range(along)]
    for turn, z in enumerate(reversed(range(along))):
        row = list(range(1, across))
        if turn % 2:
            row.reverse()
        order += [z * across + x for x in row]
    return order


def lookup(table, index):
    found = jnp.int32(0)
    for place, value in enumerate(table):
        found = found + jnp.where(index == place, jnp.int32(value), jnp.int32(0))
    return found


def kernel(
    shards, peers, order,
    q_n, q_b, k_n, v_n, k_b, v_b, off_n, off_b, residual, out_n, out_b, gain, up, down,
    o_ref,
    kv_slots, off_slots, up_slots, down_slots, mixed, part, inbox, updated, normed_all,
    product, hidden, channel, send_sems, recv_sems, tp_send, tp_recv, load_sems,
):
    tok = q_n.shape[0]
    wide = product.shape[1]
    model = part.shape[2]
    rows = residual.shape[0]
    depth = up.shape[0]
    me = lax.axis_index("sp")
    me_tp = lax.axis_index("tp")
    inverse = [order.index(s) for s in range(shards)]
    pos = lookup(inverse, me)
    right = lookup(order, lax.rem(pos + 1, shards))
    left = lookup(order, lax.rem(pos + shards - 1, shards))

    half_up, half_down = wide // 2, wide // 2
    loads = []
    for way, (k, v, off) in enumerate(((k_n, v_n, off_n), (k_b, v_b, off_b))):
        loads += [
            (k, kv_slots.at[way, 0, pl.ds(0, tok)]),
            (v, kv_slots.at[way, 0, pl.ds(tok, tok)]),
            (off, off_slots.at[way, 0]),
        ]
    for way in range(2):
        loads += [
            (up.at[:, pl.ds(way * half_up, half_up)], up_slots.at[way, 0]),
            (down.at[pl.ds(way * half_down, half_down)], down_slots.at[way, 0]),
        ]
    loads = [
        pltpu.make_async_copy(src, dst, load_sems.at[i]) for i, (src, dst) in enumerate(loads)
    ]
    for load in loads:
        load.start()

    barrier = pltpu.get_barrier_semaphore()
    for shard in (left, right):
        pl.semaphore_signal(
            barrier, inc=1, device_id=(shard, me_tp), device_id_type=pl.DeviceIdType.MESH
        )
    for d in range(1, peers):
        pl.semaphore_signal(
            barrier, inc=1, device_id=(me, lax.rem(me_tp + d, peers)),
            device_id_type=pl.DeviceIdType.MESH,
        )
    pl.semaphore_wait(barrier, 1 + peers)

    def piece(stream, way, t):
        if stream == 0:
            return off_slots.at[way, t]
        if stream in (1, 2):
            return kv_slots.at[way, t, pl.ds((stream - 1) * tok, tok)]
        if stream in (3, 4):
            size = depth // 2
            return up_slots.at[way, t, pl.ds((stream - 3) * size, size)]
        size = half_down // 2
        return down_slots.at[way, t, pl.ds((stream - 5) * size, size)]

    def hop(stream, way, t):
        return pltpu.make_async_remote_copy(
            src_ref=piece(stream, way, t),
            dst_ref=piece(stream, way, t + 1),
            send_sem=send_sems.at[way, stream, t],
            recv_sem=recv_sems.at[way, stream, t],
            device_id=((left if way else right), me_tp),
            device_id_type=pl.DeviceIdType.MESH,
        )

    def begin(streams, t):
        for stream in streams:
            for way in range(2):
                hop(stream, way, t).start()

    def relay(streams, t):
        for stream in streams:
            for way in range(2):
                hop(stream, way, t - 1).wait_recv()
                hop(stream, way, t).start()

    def arrive(streams):
        for stream in streams:
            for way in range(2):
                hop(stream, way, shards - 2).wait_recv()

    def each(first, last, body):
        def step(t, carry):
            body(t)
            return carry

        lax.fori_loop(first, last, step, 0)

    KEYS, UPS, DOWNS = (0, 1, 2), (3, 4), (5, 6)
    for load in loads:
        load.wait()
    begin(KEYS, 0)
    each(1, shards - 1, functools.partial(relay, KEYS))
    begin(UPS, 0)
    arrive(KEYS)

    row_at = lax.broadcasted_iota(jnp.int32, (tok, tok), 0)
    col_at = lax.broadcasted_iota(jnp.int32, (tok, tok), 1)
    later = (row_at > col_at).astype(BF16)
    later2 = jnp.concatenate([later, later], axis=0)
    heads = []
    for way, (q, size) in enumerate(((q_n, NARROW_SIZE), (q_b, BROAD_SIZE))):
        for h in range(q.shape[1] // size):
            heads.append((way, h, size, q))

    def head_block(way, h, size, q, block, keep_sum, diagonal):
        there = lookup(inverse, block)
        slot = lax.rem((there - pos if way else pos - there) + shards, shards)
        cols = pl.ds(h * size, size)
        keys = kv_slots[way, slot, pl.ds(0, tok), cols]
        values = kv_slots[way, slot, pl.ds(tok, tok), cols]
        offset = off_slots[way, slot].astype(F32)[h : h + 1, :]
        scores = lax.dot_general(
            q[:, cols], keys, (((1,), (1,)), ((), ())), preferred_element_type=F32
        ) * (size ** -0.5) + offset
        keep = -(jnp.maximum(scores, 0.0) + jnp.log(1.0 + jnp.exp(-jnp.abs(scores))))
        breaks = scores + keep
        if diagonal:
            keep = jnp.where(col_at < row_at, keep, 0.0)
        high = keep.astype(BF16)
        low = (keep - high.astype(F32)).astype(BF16)
        after = jnp.dot(
            jnp.concatenate([high, low], axis=1), later2, preferred_element_type=F32
        )
        weight = jnp.exp(breaks + after + keep_sum)
        if diagonal:
            weight = jnp.where(col_at < row_at, weight, 0.0)
        added = jnp.dot(weight.astype(BF16), values, preferred_element_type=F32)
        return keep_sum + (after[:, :1] + keep[:, :1]), added

    turn_up = 1
    for index, (way, h, size, q) in enumerate(heads):
        start = head_block(way, h, size, q, me, jnp.zeros((tok, 1), F32), True)

        def sweep(turn, state, way=way, h=h, size=size, q=q):
            keep_sum, running = state
            keep_sum, added = head_block(way, h, size, q, me - 1 - turn, keep_sum, False)
            return keep_sum, running + added

        _, running = lax.fori_loop(0, me, sweep, start)
        base = way * q_n.shape[1] + h * size
        mixed[:, pl.ds(base, size)] = running.astype(BF16)
        if index % 2:
            relay(UPS, turn_up)
            turn_up += 1

    def tp_copy(src, dst, kind, d):
        return pltpu.make_async_remote_copy(
            src_ref=src, dst_ref=dst,
            send_sem=tp_send.at[kind, d - 1], recv_sem=tp_recv.at[kind, d - 1],
            device_id=(me, lax.rem(me_tp + d, peers)),
            device_id_type=pl.DeviceIdType.MESH,
        )

    def scatter(kind):
        copies = []
        for d in range(1, peers):
            peer = lax.rem(me_tp + d, peers)
            copies.append(
                tp_copy(
                    part.at[kind, pl.ds(pl.multiple_of(peer * rows, rows), rows)],
                    inbox.at[kind, d - 1], kind, d,
                )
            )
        for copy in copies:
            copy.start()
        return copies

    def summed(kind, copies):
        for copy in copies:
            copy.wait_recv()
        own = pl.multiple_of(me_tp * rows, rows)
        total = part[kind, pl.ds(own, rows), :].astype(F32)
        for d in range(1, peers):
            total = total + inbox[kind, d - 1].astype(F32)
        return total

    tile = min(512, model)
    n_cols = out_n.shape[0]

    def project(c):
        cols = pl.ds(pl.multiple_of(c * tile, tile), tile)
        part[0, :, cols] = (
            jnp.dot(mixed[:, :n_cols], out_n[:, cols], preferred_element_type=F32)
            + jnp.dot(mixed[:, n_cols:], out_b[:, cols], preferred_element_type=F32)
        ).astype(BF16)

    each(0, model // tile, project)
    first = scatter(0)
    relay(UPS, turn_up)
    updated[...] = residual[...].astype(F32) + summed(0, first)
    value = updated[...]
    scale = lax.rsqrt(jnp.mean(value * value, axis=-1, keepdims=True) + 1e-06)
    mine = pl.ds(pl.multiple_of(me_tp * rows, rows), rows)
    normed_all[mine, :] = (value * scale * gain[...]).astype(BF16)
    spread = [tp_copy(normed_all.at[mine], normed_all.at[mine], 2, d) for d in range(1, peers)]
    for copy in spread:
        copy.start()
    relay(UPS, turn_up + 1)
    for copy in spread:
        copy.wait_recv()

    product[...] = jnp.zeros_like(product)
    channel[...] = jnp.zeros_like(channel)
    step_cols = min(512, half_up)

    def source(way, t):
        return lookup(order, lax.rem((pos + t if way else pos - t + shards), shards))

    def climb(t):
        for way in range(2):
            lhs_cols = pl.ds(pl.multiple_of(source(way, t) * depth, depth), depth)

            def one(c, way=way, lhs_cols=lhs_cols):
                at = pl.multiple_of(c * step_cols, step_cols)
                product[:, pl.ds(way * half_up + at, step_cols)] += jnp.dot(
                    normed_all[:, lhs_cols], up_slots[way, t, :, pl.ds(at, step_cols)],
                    preferred_element_type=F32,
                )

            each(0, half_up // step_cols, one)

    def descend(t):
        for way in range(2):
            cols = pl.ds(pl.multiple_of(source(way, t) * depth, depth), depth)
            channel[:, cols] += jnp.dot(
                hidden[:, pl.ds(way * half_down, half_down)], down_slots[way, t],
                preferred_element_type=F32,
            )

    each(0, turn_up + 2, climb)

    def up_step(t):
        relay(UPS, t)
        climb(t)

    each(turn_up + 2, shards - 1, up_step)
    begin(DOWNS, 0)
    arrive(UPS)
    climb(shards - 1)

    def activate(c):
        cols = pl.ds(pl.multiple_of(c * step_cols, step_cols), step_cols)
        hidden[:, cols] = jnp.square(jnp.maximum(product[:, cols], 0.0)).astype(BF16)

    each(0, wide // step_cols, activate)
    descend(0)

    def down_step(t):
        relay(DOWNS, t)
        descend(t)

    each(1, shards - 1, down_step)
    arrive(DOWNS)
    descend(shards - 1)

    def settle(c):
        cols = pl.ds(pl.multiple_of(c * tile, tile), tile)
        part[1, :, cols] = channel[:, cols].astype(BF16)

    each(0, model // tile, settle)
    last = scatter(1)
    o_ref[...] = (updated[...] + summed(1, last)).astype(BF16)

    def drain(t):
        for stream in KEYS + UPS + DOWNS:
            for way in range(2):
                hop(stream, way, t).wait_send()

    each(0, shards - 1, drain)
    for copy in first + spread + last:
        copy.wait_send()


def local(
    shards, peers, order,
    query_narrow, key_narrow, value_narrow, query_broad, key_broad, value_broad,
    offset_narrow, offset_broad, residual, out_narrow, out_broad, norm_gain, up_proj, down_proj,
):
    tok, columns = query_narrow.shape
    rows, model = residual.shape
    depth, wide = up_proj.shape
    pad = 16

    def padded(offset):
        return jnp.pad(offset, ((0, pad - offset.shape[0]), (0, 0)))

    vmem = pl.BlockSpec(memory_space=pltpu.VMEM)
    anywhere = pl.BlockSpec(memory_space=pl.ANY)
    return pl.pallas_call(
        functools.partial(kernel, shards, peers, order),
        out_shape=jax.ShapeDtypeStruct((rows, model), BF16),
        in_specs=[vmem] * 2 + [anywhere] * 6 + [vmem] * 4 + [anywhere] * 2,
        out_specs=vmem,
        scratch_shapes=[
            pltpu.VMEM((2, shards, 2 * tok, columns), BF16),
            pltpu.VMEM((2, shards, pad, tok), BF16),
            pltpu.VMEM((2, shards, depth, wide // 2), BF16),
            pltpu.VMEM((2, shards, wide // 2, depth), BF16),
            pltpu.VMEM((tok, 2 * columns), BF16),
            pltpu.VMEM((2, tok, model), BF16),
            pltpu.VMEM((2, peers - 1, rows, model), BF16),
            pltpu.VMEM((rows, model), F32),
            pltpu.VMEM((tok, model), BF16),
            pltpu.VMEM((tok, wide), F32),
            pltpu.VMEM((tok, wide), BF16),
            pltpu.VMEM((tok, model), F32),
            pltpu.SemaphoreType.DMA((2, 7, shards)),
            pltpu.SemaphoreType.DMA((2, 7, shards)),
            pltpu.SemaphoreType.DMA((3, peers - 1)),
            pltpu.SemaphoreType.DMA((3, peers - 1)),
            pltpu.SemaphoreType.DMA((10,)),
        ],
        compiler_params=pltpu.CompilerParams(
            collective_id=0, has_side_effects=True, vmem_limit_bytes=60 << 20
        ),
    )(
        query_narrow, query_broad, key_narrow, value_narrow, key_broad, value_broad,
        padded(offset_narrow), padded(offset_broad), residual, out_narrow, out_broad,
        norm_gain.reshape(1, -1), up_proj, down_proj,
    )


def solution(mesh):
    shards, peers = mesh.shape["sp"], mesh.shape["tp"]
    return jax.shard_map(
        functools.partial(local, shards, peers, tuple(ring_order(shards))),
        mesh=mesh,
        in_specs=(
            P("sp", "tp"),
            P("sp", "tp"),
            P("sp", "tp"),
            P("sp", "tp"),
            P("sp", "tp"),
            P("sp", "tp"),
            P("tp", "sp"),
            P("tp", "sp"),
            P(("sp", "tp"), None),
            P("tp", None),
            P("tp", None),
            P(),
            P("sp", "tp"),
            P("tp", "sp"),
        ),
        out_specs=P(("sp", "tp"), None),
        check_vma=False,
    )
```
